32 devices in a mesh: ep: 16 (over z, x, core), tp: 2 (over y).
Axes of the slice: x: 2, y: 2, z: 4, core: 2. Of those that a mesh axis runs over, the one named last changes fastest.
Arguments:
- tokens: bfloat16 [192, 1024], P('ep'), may hold values from -6 to 6
- norm_gain: float32 [1024], replicated, may hold values from 0.1 to 1.9
- w_query: bfloat16 [1024, 512], P(None, 'tp'), may hold values from -0.1875 to 0.1875
- w_key: bfloat16 [1024, 512], P(None, 'tp'), may hold values from -0.1875 to 0.1875
- w_value: bfloat16 [1024, 512], P(None, 'tp'), may hold values from -0.1875 to 0.1875
- w_input_gate: bfloat16 [1024, 4], replicated, may hold values from -0.1875 to 0.1875
- w_forget_gate: bfloat16 [1024, 4], replicated, may hold values from -0.1875 to 0.1875
- input_bias: float32 [4], replicated, may hold values from -2 to 1
- forget_bias: float32 [4], replicated, may hold values from 0 to 4
- state_c: float32 [192, 4, 128, 128], P('ep', 'tp'), may hold values from -1.75 to 1.75
- state_n: float32 [192, 4, 128], P('ep', 'tp'), may hold values from -1.75 to 1.75
- state_m: float32 [192, 4], P('ep', 'tp'), may hold values from -1 to 2
- w_mixer_out: bfloat16 [512, 1024], P('tp'), may hold values from -0.25 to 0.25
- ffn_gain: float32 [1024], replicated, may hold values from 0.1 to 1.9
- routes: int32 [192, 6], P('ep'), may hold values from 0 to 15, all different within a row; in each aligned block of 12 rows (0 to 11, 12 to 23, ...) at most 10 rows name the same one
- route_scale: bfloat16 [192, 6], P('ep'), may hold values from 0.099609375 to 1
- w_expert_gate: bfloat16 [16, 1024, 1024], P('ep', None, 'tp'), may hold values from -0.375 to 0.375
- w_expert_up: bfloat16 [16, 1024, 1024], P('ep', None, 'tp'), may hold values from -0.375 to 0.375
- w_expert_down: bfloat16 [16, 1024, 1024], P('ep', 'tp'), may hold values from -0.1875 to 0.1875
- w_dense_gate: bfloat16 [1024, 512], P(None, 'tp'), may hold values from -0.1875 to 0.1875
- w_dense_up: bfloat16 [1024, 512], P(None, 'tp'), may hold values from -0.1875 to 0.1875
- w_dense_down: bfloat16 [512, 1024], P('tp'), may hold values from -0.5 to 0.5
- w_branch_gate: bfloat16 [1024], replicated, may hold values from -0.1875 to 0.1875
Outputs:
- output: bfloat16 [192, 1024], P('ep', 'tp')
- new_c: float32 [192, 4, 128, 128], P('ep', 'tp')
- new_n: float32 [192, 4, 128], P('ep', 'tp')
- new_m: float32 [192, 4], P('ep', 'tp')
The draws below stay inside these ranges and needn't reach their ends.
Inputs may be any that keep to these rules, and one draw needn't show every extreme that they name: `routes`: each row names 6 different experts. Among the rows of one index of ep no expert is named by more than 10 rows, a bound that some block reaches of them.
All inputs are finite; a program needn't handle non-finite values.
Results may differ from the reference program's by a relative error of at most 0.018.
Values may be sent and summed in bfloat16 or wider, within the bound.
No kernel may reach another device: no remote copies, remote signals or barrier semaphores. Data moves between devices by JAX's collectives and lax.ppermute only.
A program may use at most 64 MiB of HBM per device.

```python
import math
import jax
import jax.numpy as jnp
import numpy as np
from jax import lax

D = 1024
HEADS = 4
DQK = 128
DV = 128
D_EXPERT = 1024
DENSE_FF = 512
TOP_K = 6
SEQ_DEV = 12
EXPERTS = 16
TOKENS = 192
CAP = 10
N_TP = 2


def block_scale(rng, dims, split, low, top_value):
    gain = 1.0
    for dim, parts in split:
        draws = jax.random.uniform(jax.random.fold_in(jax.random.fold_in(rng, 6), dim), (parts,), jnp.float32, low / len(split), top_value / len(split))
        gain = gain * jnp.repeat(jnp.exp(draws), dims[dim] // parts).reshape((-1,) + (1,) * (len(dims) - 1 - dim))
    return gain


def assign_block(rng, own, number, rows, count, top, most, slope):
    sequence = jax.random.permutation(rng, count)
    crowded, common = shares(count, rows * top, most, slope, True), shares(count, rows * top, most, slope, False)
    places = jnp.arange(count)

    def named(sizes, turn):
        used = int((sizes > 0).sum())
        fixed = max(1, used // 4)
        moved = fixed + (places - fixed + turn * (used - fixed)) % max(1, count - fixed)
        return jnp.zeros((count,), jnp.int32).at[sequence[jnp.where(places < fixed, places, moved)]].set(jnp.asarray(sizes, jnp.int32))

    sizes = jnp.where(number % 4 == 0, named(crowded, number // 4), named(common, number - number // 4 - 1))
    mixed = jax.random.permutation(jax.random.fold_in(own, 3), count)
    donor, taker = mixed[0:count // 2 * 2:2], mixed[1:count // 2 * 2:2]
    room = jnp.minimum(sizes[donor] - 1, most - sizes[taker]) // 2
    room = jnp.where((donor == sequence[0]) | (taker == sequence[0]) | (sizes[taker] == 0), 0, jnp.maximum(room, 0))
    moved = jax.random.randint(jax.random.fold_in(own, 4), (count // 2,), 0, 1 << 20) % (room + 1)
    sizes = sizes.at[donor].add(-moved).at[taker].add(moved)
    members = jnp.searchsorted(jnp.cumsum(sizes), jnp.arange(rows * top), side="right").astype(jnp.int32)
    listing = members.reshape(top, rows).T
    listing = listing[jax.random.permutation(jax.random.fold_in(own, 1), rows)]
    turn = jax.random.randint(jax.random.fold_in(own, 2), (rows, 1), 0, top)
    return jnp.take_along_axis(listing, (jnp.arange(top)[None, :] + turn) % top, axis=1)


def shares(number_of, total, most, lean, full):
    weights = [(1 << 20) // math.isqrt(standing ** lean) + 1 for standing in range(1, number_of + 1)]
    largest = most if full else min(most, max(-(-total // number_of), total * weights[0] // sum(weights)))
    least = 1 if total - largest >= number_of - 1 else 0
    given, surplus = [largest] + [least] * (number_of - 1), total - largest - least * (number_of - 1)
    while surplus > 0:
        free = [i for i in range(1, number_of) if given[i] < largest] or [i for i in range(1, number_of) if given[i] < most]
        whole, left = sum([weights[i] for i in free]), surplus
        for i in free:
            extra = min(most - given[i], max(1, left * weights[i] // whole), surplus)
            given[i] = given[i] + extra
            surplus = surplus - extra
    return np.array(given)


def scatter_about(own_key, shape, spread, limit, pieces=(), kind=jnp.bfloat16):
    array = jax.random.normal(own_key, shape, jnp.float32) * spread
    if len(pieces) > 0:
        array = block_scale(own_key, shape, pieces, -0.22, 0.18) * array
    return jnp.clip(array, min=-limit, max=limit).astype(kind)


def setup_inputs(seed: int = 0) -> dict:
    key_list = jax.random.split(jax.random.key(seed), 24)
    tokens = scatter_about(key_list[0], (TOKENS, D), 1.0, 6.0, ((0, 16),))
    norm_gain = jnp.clip(1.0 + 0.18 * jax.random.normal(key_list[1], (D,), jnp.float32), 0.1, 1.9)
    w_query = scatter_about(key_list[2], (D, HEADS * DQK), D ** -0.5, 0.1875, ((1, 2),))
    w_key = scatter_about(key_list[3], (D, HEADS * DQK), D ** -0.5, 0.1875, ((1, 2),))
    w_value = scatter_about(key_list[4], (D, HEADS * DV), D ** -0.5, 0.1875, ((1, 2),))
    w_input_gate = scatter_about(key_list[5], (D, HEADS), D ** -0.5, 0.1875)
    w_forget_gate = scatter_about(key_list[6], (D, HEADS), D ** -0.5, 0.1875)
    input_bias = jnp.clip(jax.random.uniform(key_list[7], (HEADS,), jnp.float32, -2.0, 1.0), -2.0, 1.0)
    forget_bias = jnp.clip(jax.random.uniform(key_list[8], (HEADS,), jnp.float32, 0.0, 4.0), 0.0, 4.0)
    state_c = scatter_about(key_list[9], (TOKENS, HEADS, DQK, DV), 0.3, 1.75, ((0, 16), (1, 2)), jnp.float32)
    state_n = scatter_about(key_list[10], (TOKENS, HEADS, DQK), 0.3, 1.75, ((0, 16), (1, 2)), jnp.float32)
    state_m = jnp.clip(-1.0 + 3.0 * jax.random.uniform(key_list[11], (TOKENS, HEADS), jnp.float32) ** block_scale(key_list[11], (TOKENS, HEADS), ((0, 16), (1, 2)), -0.2, 0.2), -1.0, 2.0)
    w_mixer_out = scatter_about(key_list[12], (HEADS * DV, D), (HEADS * DV) ** -0.5, 0.25, ((0, 2),))
    ffn_gain = jnp.clip(1.0 + 0.18 * jax.random.normal(key_list[13], (D,), jnp.float32), 0.1, 1.9)
    routes_keys = jax.random.split(jax.random.fold_in(key_list[14], 1), TOKENS // SEQ_DEV)
    routes_turns = jax.random.permutation(jax.random.fold_in(key_list[14], 3), TOKENS // SEQ_DEV)
    routes = jax.vmap(lambda own, number: assign_block(jax.random.fold_in(key_list[14], 2), own, number, SEQ_DEV, EXPERTS, TOP_K, CAP, 2))(routes_keys, routes_turns).reshape((TOKENS, TOP_K))
    route_scale = jnp.clip(jnp.exp(math.log(1.0) - 2.306499 * jax.random.uniform(key_list[15], (TOKENS, TOP_K), jnp.float32) ** block_scale(key_list[15], (TOKENS, TOP_K), ((0, 16),), -0.2, 0.2)), 0.099609375, 1.0).astype(jnp.bfloat16)
    w_expert_gate = scatter_about(key_list[16], (EXPERTS, D, D_EXPERT), (2.0 * D ** -0.5), 0.375, ((0, 16), (2, 2)))
    w_expert_up = scatter_about(key_list[17], (EXPERTS, D, D_EXPERT), (2.0 * D ** -0.5), 0.375, ((0, 16), (2, 2)))
    w_expert_down = scatter_about(key_list[18], (EXPERTS, D_EXPERT, D), D_EXPERT ** -0.5, 0.1875, ((0, 16), (1, 2)))
    w_dense_gate = scatter_about(key_list[19], (D, DENSE_FF), D ** -0.5, 0.1875, ((1, 2),))
    w_dense_up = scatter_about(key_list[20], (D, DENSE_FF), D ** -0.5, 0.1875, ((1, 2),))
    w_dense_down = scatter_about(key_list[21], (DENSE_FF, D), (DENSE_FF // 4) ** -0.5, 0.5, ((0, 2),))
    w_branch_gate = scatter_about(key_list[22], (D,), D ** -0.5, 0.1875)
    return {"tokens": tokens, "norm_gain": norm_gain, "w_query": w_query, "w_key": w_key, "w_value": w_value, "w_input_gate": w_input_gate, "w_forget_gate": w_forget_gate, "input_bias": input_bias, "forget_bias": forget_bias, "state_c": state_c, "state_n": state_n, "state_m": state_m, "w_mixer_out": w_mixer_out, "ffn_gain": ffn_gain, "routes": routes, "route_scale": route_scale, "w_expert_gate": w_expert_gate, "w_expert_up": w_expert_up, "w_expert_down": w_expert_down, "w_dense_gate": w_dense_gate, "w_dense_up": w_dense_up, "w_dense_down": w_dense_down, "w_branch_gate": w_branch_gate}


EPSILON = 1e-06
CLAMP_LIMIT = 7.0
SWISH_ALPHA = 1.702

def stored(values):
    return lax.optimization_barrier(values.astype(jnp.bfloat16)).astype(jnp.float32)

def rms_scaled(values, gain_vec):
    values = values.astype(jnp.float32)
    scaled = values * lax.rsqrt(lax.optimization_barrier(jnp.mean(values * values, axis=-1, keepdims=True)) + EPSILON)
    return scaled * gain_vec.astype(jnp.float32)

def slot_tables(route_blocks, expert_ids, weight_blocks, capacity, top_count):
    entries = route_blocks.shape[1]
    matched = (route_blocks[:, None, :] == expert_ids[None, :, None]).astype(jnp.int32)
    ranking = jnp.cumsum(matched, axis=2, dtype=jnp.int32) - 1
    slot_ids = jnp.arange(capacity, dtype=jnp.int32)
    chosen = (matched[:, :, None, :] == 1) & (ranking[:, :, None, :] == slot_ids[None, None, :, None])
    slot_hot = jnp.where(chosen, 1.0, 0.0).astype(jnp.float32)
    entry_ids = jnp.arange(entries, dtype=jnp.int32)
    token_ids = jnp.arange(entries // top_count, dtype=jnp.int32)
    owner = jnp.where(entry_ids[:, None] // top_count == token_ids[None, :], 1.0, 0.0).astype(jnp.float32)
    token_hot = jnp.einsum('becj,js->becs', slot_hot, owner, precision=lax.Precision.HIGHEST)
    slot_weight = jnp.einsum('becj,bj->bec', slot_hot, weight_blocks, precision=lax.Precision.HIGHEST)
    return (token_hot, slot_weight)

def reference(tokens, norm_gain, w_query, w_key, w_value, w_input_gate, w_forget_gate, input_bias, forget_bias, state_c, state_n, state_m, w_mixer_out, ffn_gain, routes, route_scale, w_expert_gate, w_expert_up, w_expert_down, w_dense_gate, w_dense_up, w_dense_down, w_branch_gate):
    row_count = tokens.shape[0]
    normed = rms_scaled(tokens, norm_gain).astype(jnp.bfloat16)
    queries = stored(jnp.dot(normed, w_query, preferred_element_type=jnp.float32)).reshape(row_count, HEADS, DQK)
    key_rows = stored(jnp.dot(normed, w_key, preferred_element_type=jnp.float32)).reshape(row_count, HEADS, DQK)
    value_rows = stored(jnp.dot(normed, w_value, preferred_element_type=jnp.float32)).reshape(row_count, HEADS, DV)
    input_pre = jnp.dot(normed, w_input_gate, preferred_element_type=jnp.float32) + input_bias
    forget_log = jax.nn.log_sigmoid(jnp.dot(normed, w_forget_gate, preferred_element_type=jnp.float32) + forget_bias)
    new_m = jnp.maximum(forget_log + state_m, input_pre)
    forget_factor = jnp.exp(forget_log + state_m - new_m)
    input_factor = jnp.exp(input_pre - new_m)
    key_scaled = key_rows * DQK ** (-0.5)
    new_c = forget_factor[..., None, None] * state_c + input_factor[..., None, None] * (key_scaled[..., :, None] * value_rows[..., None, :])
    new_n = forget_factor[..., None] * state_n + input_factor[..., None] * key_scaled
    numer = jnp.einsum('thd,thdv->thv', queries, new_c, precision=lax.Precision.HIGHEST)
    denom = jnp.einsum('thd,thd->th', queries, new_n, precision=lax.Precision.HIGHEST)
    head_out = (numer / jnp.maximum(jnp.abs(denom), 1.0)[..., None]).astype(jnp.bfloat16).reshape(row_count, HEADS * DV)
    group_width = HEADS // N_TP * DV
    mixer_total = jnp.zeros((row_count, D), jnp.float32)
    for group in range(N_TP):
        lower = group * group_width
        mixer_total = mixer_total + stored(jnp.dot(head_out[:, lower:lower + group_width], w_mixer_out[lower:lower + group_width], preferred_element_type=jnp.float32))
    mixer_out = mixer_total.astype(jnp.bfloat16)
    residual = tokens.astype(jnp.float32) + mixer_out.astype(jnp.float32)
    ffn_in = rms_scaled(residual, ffn_gain).astype(jnp.bfloat16)
    scale_values = route_scale.astype(jnp.float32)
    route_weight = scale_values / lax.optimization_barrier(jnp.sum(scale_values, axis=1, keepdims=True))
    block_count = row_count // SEQ_DEV
    route_blocks = routes.reshape(block_count, SEQ_DEV * TOP_K)
    weight_blocks = route_weight.reshape(block_count, SEQ_DEV * TOP_K)
    token_blocks = ffn_in.astype(jnp.float32).reshape(block_count, SEQ_DEV, D)
    part_width = D_EXPERT // N_TP

    def one_expert(total, inputs):
        gate_weight, up_weight, down_weight, expert = inputs
        token_hot, slot_weight = slot_tables(route_blocks, expert[None], weight_blocks, CAP, TOP_K)
        token_hot = token_hot[:, 0]
        slot_weight = slot_weight[:, 0]
        slot_rows = jnp.einsum('bcs,bsd->bcd', token_hot, token_blocks, precision=lax.Precision.HIGHEST).astype(jnp.bfloat16).reshape(block_count * CAP, D)
        gate_pre = jnp.minimum(jnp.dot(slot_rows, gate_weight, preferred_element_type=jnp.float32), CLAMP_LIMIT)
        up_pre = jnp.clip(jnp.dot(slot_rows, up_weight, preferred_element_type=jnp.float32), -CLAMP_LIMIT, CLAMP_LIMIT)
        hidden = (gate_pre * jax.nn.sigmoid(SWISH_ALPHA * gate_pre) * (up_pre + 1.0)).astype(jnp.bfloat16)
        expert_out = jnp.zeros((block_count * CAP, D), jnp.float32)
        for part in range(N_TP):
            lower = part * part_width
            expert_out = expert_out + stored(jnp.dot(hidden[:, lower:lower + part_width], down_weight[lower:lower + part_width], preferred_element_type=jnp.float32))
        weighted = expert_out.reshape(block_count, CAP, D) * slot_weight[..., None]
        total = total + jnp.einsum('bcs,bcd->bsd', token_hot, weighted, precision=lax.Precision.HIGHEST)
        return (total, None)
    moe, _ = lax.scan(one_expert, jnp.zeros((block_count, SEQ_DEV, D), jnp.float32), (w_expert_gate, w_expert_up, w_expert_down, jnp.arange(EXPERTS, dtype=jnp.int32)))
    dense_gate_pre = jnp.dot(ffn_in, w_dense_gate, preferred_element_type=jnp.float32)
    dense_hidden = (jax.nn.silu(dense_gate_pre) * jnp.dot(ffn_in, w_dense_up, preferred_element_type=jnp.float32)).astype(jnp.bfloat16)
    dense = jnp.dot(dense_hidden, w_dense_down, preferred_element_type=jnp.float32)
    branch_weight = jax.nn.sigmoid(jnp.dot(ffn_in, w_branch_gate, preferred_element_type=jnp.float32))
    output = (residual + moe.reshape(row_count, D) + branch_weight[:, None] * dense).astype(jnp.bfloat16)
    return (output, new_c, new_n, new_m)
```

```python
import functools
import jax
import jax.numpy as jnp
from jax import lax
from jax.experimental import pallas as pl
from jax.experimental.pallas import tpu as pltpu
from jax.sharding import PartitionSpec as P

EPSILON = 1e-06
CLAMP_LIMIT = 7.0
SWISH_ALPHA = 1.702
AXES = ("ep", "tp")
LANES = 128
F32 = jnp.float32
BF16 = jnp.bfloat16


def dot(a, b):
    return jnp.dot(a, b, preferred_element_type=F32)


def cell_kernel(
    place,
    tokens,
    gain,
    w_query,
    w_key,
    w_value,
    w_in,
    w_forget,
    bias_in,
    bias_forget,
    state_c,
    state_n,
    state_m,
    w_mixer,
    part,
    new_c,
    new_n,
    new_m,
    numer,
):
    rows = tokens.shape[0]
    heads, dk, dv = state_c.shape[1:]
    x = tokens[...].astype(F32)
    normed = x * lax.rsqrt(jnp.mean(x * x, axis=-1, keepdims=True) + EPSILON)
    normed = (normed * gain[...]).astype(BF16)
    queries = dot(normed, w_query[...]).astype(BF16).astype(F32)
    keys = dot(normed, w_key[...]).astype(BF16).astype(F32) * dk ** (-0.5)
    values = dot(normed, w_value[...]).astype(BF16).astype(F32)
    in_all = dot(normed, w_in[...]) + bias_in[...]
    forget_all = dot(normed, w_forget[...]) + bias_forget[...]
    groups = in_all.shape[1] // heads
    in_pre = in_all[:, :heads]
    forget_pre = forget_all[:, :heads]
    for g in range(1, groups):
        here = place[0] == g
        in_pre = jnp.where(here, in_all[:, g * heads : (g + 1) * heads], in_pre)
        forget_pre = jnp.where(here, forget_all[:, g * heads : (g + 1) * heads], forget_pre)
    forget_log = jnp.minimum(forget_pre, 0.0) - jnp.log1p(jnp.exp(-jnp.abs(forget_pre)))
    carried = forget_log + state_m[...]
    top = jnp.maximum(carried, in_pre)
    new_m[...] = top
    forget = jnp.exp(carried - top)
    enter = jnp.exp(in_pre - top)
    scales = []
    for h in range(heads):
        q = queries[:, h * dk : (h + 1) * dk]
        k = keys[:, h * dk : (h + 1) * dk]
        v = values[:, h * dv : (h + 1) * dv]
        f = jnp.broadcast_to(forget[:, h : h + 1], (rows, dv))
        iv = enter[:, h : h + 1] * v
        nn = forget[:, h : h + 1] * state_n[:, h, :] + enter[:, h : h + 1] * k
        new_n[:, h, :] = nn
        denom = jnp.sum(q * nn, axis=-1, keepdims=True)
        scales.append(jnp.maximum(jnp.abs(denom), 1.0))
        pad = jnp.zeros((LANES - rows, dk), F32)
        q_t = jnp.concatenate([q, pad], axis=0).T
        k_t = jnp.concatenate([k, pad], axis=0).T
        for t in range(rows):
            c = f[t : t + 1] * state_c[t, h] + k_t[:, t : t + 1] * iv[t : t + 1]
            new_c[t, h] = c
            numer[t : t + 1, h * dv : (h + 1) * dv] = jnp.sum(
                q_t[:, t : t + 1] * c, axis=0, keepdims=True
            )
    head_out = jnp.concatenate(
        [numer[:, h * dv : (h + 1) * dv] / scales[h] for h in range(heads)], axis=1
    ).astype(BF16)
    part[...] = dot(head_out, w_mixer[...]).astype(BF16)


def cell(place, *arrays):
    tokens = arrays[0]
    state_c, state_n, state_m = arrays[9:12]
    rows, width = tokens.shape
    heads, dv = state_c.shape[1], state_c.shape[3]
    vmem = pl.BlockSpec(memory_space=pltpu.VMEM)
    return pl.pallas_call(
        cell_kernel,
        out_shape=(
            jax.ShapeDtypeStruct((rows, width), BF16),
            jax.ShapeDtypeStruct(state_c.shape, F32),
            jax.ShapeDtypeStruct(state_n.shape, F32),
            jax.ShapeDtypeStruct(state_m.shape, F32),
        ),
        in_specs=[pl.BlockSpec(memory_space=pltpu.SMEM)] + [vmem] * len(arrays),
        out_specs=[vmem] * 4,
        scratch_shapes=[pltpu.VMEM((rows, heads * dv), F32)],
        name="cell",
    )(place, *arrays)


def expert_kernel(
    count, top, place, near, far, w_gate, w_up, w_down, w_dgate, w_dup, w_ddown, w_branch, send, keep
):
    half = near.shape[0]
    width = w_gate.shape[0]
    tp, _, cols = keep.shape
    packed = jnp.concatenate([far[...], near[...]], axis=0)
    rows = packed[:, :width]
    extra = packed[:, width:].astype(F32)
    own = place[1].astype(F32)
    lane = lax.broadcasted_iota(jnp.int32, extra.shape, 1)
    scale = pltpu.roll(extra, LANES // 2, 1)
    valid = lane < top
    total = jnp.sum(jnp.where(valid, scale, 0.0), axis=1, keepdims=True)
    mine = jnp.sum(jnp.where(valid & (extra == own), scale, 0.0), axis=1, keepdims=True)
    weight = mine / total
    gate = jnp.minimum(dot(rows, w_gate[...]), CLAMP_LIMIT)
    up = jnp.clip(dot(rows, w_up[...]), -CLAMP_LIMIT, CLAMP_LIMIT)
    hidden = (gate * jax.nn.sigmoid(SWISH_ALPHA * gate) * (up + 1.0)).astype(BF16)
    mine_rows = near[:count, :width]
    dgate = dot(mine_rows, w_dgate[...])
    dhid = (dgate * jax.nn.sigmoid(dgate) * dot(mine_rows, w_dup[...])).astype(BF16)
    branch = jax.nn.sigmoid(
        jnp.sum(mine_rows.astype(F32) * w_branch[...].astype(F32), axis=1, keepdims=True)
    )
    for h in range(tp):
        at = pl.multiple_of((place[0] ^ h) * cols, LANES)
        piece = dot(hidden, w_down[:, pl.ds(at, cols)]) * weight
        send[h] = piece[:half].astype(BF16)
        keep[h] = piece[half:]
        keep[h, :count] += branch * dot(dhid, w_ddown[:, pl.ds(at, cols)])


def experts(place, count, top, tp, near, far, *weights):
    half = near.shape[0]
    cols = weights[2].shape[1] // tp
    vmem = pl.BlockSpec(memory_space=pltpu.VMEM)
    return pl.pallas_call(
        functools.partial(expert_kernel, count, top),
        out_shape=(
            jax.ShapeDtypeStruct((tp, half, cols), BF16),
            jax.ShapeDtypeStruct((tp, half, cols), F32),
        ),
        in_specs=[pl.BlockSpec(memory_space=pltpu.SMEM)] + [vmem] * (2 + len(weights)),
        out_specs=[vmem] * 2,
        name="experts",
    )(place, near, far, *weights)


def bits_of(size):
    return [1 << b for b in range(size.bit_length() - 1)]


def combos(bits):
    masks = [0]
    for bit in bits:
        masks = masks + [m ^ bit for m in masks]
    return masks


def hop(x, ep_mask, tp_mask):
    ep, tp = lax.axis_size("ep"), lax.axis_size("tp")
    pairs = [
        (e * tp + t, (e ^ ep_mask) * tp + (t ^ tp_mask)) for e in range(ep) for t in range(tp)
    ]
    return lax.ppermute(x, AXES, pairs)


def local(
    tokens,
    norm_gain,
    w_query,
    w_key,
    w_value,
    w_input_gate,
    w_forget_gate,
    input_bias,
    forget_bias,
    state_c,
    state_n,
    state_m,
    w_mixer_out,
    ffn_gain,
    routes,
    route_scale,
    w_expert_gate,
    w_expert_up,
    w_expert_down,
    w_dense_gate,
    w_dense_up,
    w_dense_down,
    w_branch_gate,
):
    count, width = tokens.shape
    top = routes.shape[1]
    tp, ep = lax.axis_size("tp"), lax.axis_size("ep")
    tp_index, ep_index = lax.axis_index("tp"), lax.axis_index("ep")
    cols = width // tp
    place = jnp.stack([tp_index, ep_index]).astype(jnp.int32)
    part, new_c, new_n, new_m = cell(
        place,
        tokens,
        norm_gain.reshape(1, width),
        w_query,
        w_key,
        w_value,
        w_input_gate,
        w_forget_gate,
        input_bias.reshape(1, -1),
        forget_bias.reshape(1, -1),
        state_c,
        state_n,
        state_m,
        w_mixer_out,
    )
    total = part.astype(F32)
    for mask in combos(bits_of(tp))[1:]:
        total = total + hop(part, 0, mask).astype(F32)
    residual = tokens.astype(F32) + total.astype(BF16).astype(F32)
    scaled = residual * lax.rsqrt(
        jnp.mean(residual * residual, axis=-1, keepdims=True) + EPSILON
    )
    ffn_in = (scaled * ffn_gain).astype(BF16)
    blank = jnp.zeros((count, LANES // 2 - top), BF16)
    extra = jnp.concatenate([routes.astype(BF16), blank, route_scale, blank], axis=1)
    near = jnp.concatenate([ffn_in, extra], axis=1)
    rest = bits_of(ep)[1:]
    x_bits = rest[: len(rest) % 2 or 2]
    groups = [x_bits] + [rest[i : i + 2] for i in range(len(x_bits), len(rest), 2)]
    for bits in reversed(groups):
        near = jnp.concatenate([near] + [hop(near, m, 0) for m in combos(bits)[1:]], axis=0)
    far = hop(near, 1, 0)
    send, keep = experts(
        place,
        count,
        top,
        tp,
        near,
        far,
        w_expert_gate[0],
        w_expert_up[0],
        w_expert_down[0],
        w_dense_gate,
        w_dense_up,
        w_dense_down,
        w_branch_gate.reshape(1, width),
    )
    total = keep + hop(send, 1, 0).astype(F32)
    dims = [[(0, m) for m in combos(bits_of(tp))]]
    dims += [[(m, 0) for m in combos(bits)] for bits in groups]
    total = total.reshape([len(d) for d in dims] + [count, cols])
    while dims:
        masks = dims.pop(0)
        if dims and len(masks) == 2 and len(dims[0]) == 2:
            inner = dims.pop(0)
            masks = [(a[0] ^ b[0], a[1] ^ b[1]) for a in masks for b in inner]
            total = total.reshape((4,) + total.shape[2:])
        kept = total[0]
        for i in range(1, len(masks)):
            kept = kept + hop(total[i].astype(BF16), *masks[i]).astype(F32)
        total = kept
    residual_cols = lax.dynamic_slice_in_dim(residual, tp_index * cols, cols, 1)
    output = (residual_cols + total).astype(BF16)
    return (output, new_c, new_n, new_m)


def solution(mesh):
    in_specs = (
        P("ep", None),
        P(),
        P(None, "tp"),
        P(None, "tp"),
        P(None, "tp"),
        P(),
        P(),
        P(),
        P(),
        P("ep", "tp", None, None),
        P("ep", "tp", None),
        P("ep", "tp"),
        P("tp", None),
        P(),
        P("ep", None),
        P("ep", None),
        P("ep", None, "tp"),
        P("ep", None, "tp"),
        P("ep", "tp", None),
        P(None, "tp"),
        P(None, "tp"),
        P("tp", None),
        P(),
    )
    out_specs = (P("ep", "tp"), P("ep", "tp", None, None), P("ep", "tp", None), P("ep", "tp"))
    return jax.shard_map(local, mesh=mesh, in_specs=in_specs, out_specs=out_specs, check_vma=False)
```

```python
import functools
import jax
import jax.numpy as jnp
from jax import lax
from jax.experimental import pallas as pl
from jax.experimental.pallas import tpu as pltpu
from jax.sharding import PartitionSpec as P

EPSILON = 1e-06
CLAMP_LIMIT = 7.0
SWISH_ALPHA = 1.702
AXES = ("ep", "tp")
LANES = 128
F32 = jnp.float32
BF16 = jnp.bfloat16


def dot(a, b):
    return jnp.dot(a, b, preferred_element_type=F32)


def across(a, b):
    return lax.dot_general(a, b, (((1,), (1,)), ((), ())), preferred_element_type=F32)


def own_rows(both, heads):
    mine = both[:heads]
    for g in range(1, both.shape[0] // heads):
        mine = jnp.where(
            lax.axis_index("tp") == g, both[g * heads : (g + 1) * heads], mine
        )
    return mine


def bias_rows(bias, heads, rows):
    first = lax.axis_index("tp") * heads
    at = lax.broadcasted_iota(jnp.int32, (heads, rows), 0)
    out = jnp.full((heads, rows), bias[first], F32)
    for h in range(1, heads):
        out = jnp.where(at == h, bias[first + h], out)
    return out


def fetch(sources, targets, sems):
    copies = [
        pltpu.make_async_copy(a, b, sems.at[i])
        for i, (a, b) in enumerate(zip(sources, targets))
    ]
    for copy in copies:
        copy.start()
    return copies


def cell_kernel(bias_in, bias_forget, *refs):
    count = (len(refs) - 8) // 2
    sources = refs[:count]
    part, new_n, new_m, key_cols, value_rows, forget_rows = refs[count : count + 6]
    targets = refs[count + 6 : 2 * count + 6]
    numer, sems = refs[2 * count + 6 :]
    (
        tokens,
        gain,
        w_in,
        w_forget,
        state_m,
        w_query,
        w_key,
        w_value,
        state_n,
        state_c,
        w_mixer,
    ) = targets
    copies = fetch(sources, targets, sems)
    rows = tokens.shape[0]
    heads, dk, dv = state_c.shape[1:]
    for copy in copies[:2]:
        copy.wait()
    x = tokens[...].astype(F32)
    normed = x * lax.rsqrt(jnp.mean(x * x, axis=-1, keepdims=True) + EPSILON)
    normed = (normed * gain[...]).astype(BF16)
    for copy in copies[2:5]:
        copy.wait()
    in_pre = own_rows(across(w_in[...], normed), heads) + bias_rows(bias_in, heads, rows)
    forget_pre = own_rows(across(w_forget[...], normed), heads) + bias_rows(
        bias_forget, heads, rows
    )
    copies[5].wait()
    queries = dot(normed, w_query[...]).astype(BF16).astype(F32)
    copies[6].wait()
    keys = dot(normed, w_key[...]).astype(BF16).astype(F32) * dk ** (-0.5)
    copies[7].wait()
    values = dot(normed, w_value[...]).astype(BF16).astype(F32)
    for copy in copies[8:10]:
        copy.wait()
    forget_log = jnp.minimum(forget_pre, 0.0) - jnp.log1p(jnp.exp(-jnp.abs(forget_pre)))
    carried = forget_log + state_m[...]
    top = jnp.maximum(carried, in_pre)
    new_m[...] = top
    gates = jnp.concatenate([jnp.exp(carried - top), jnp.exp(in_pre - top)], axis=0)
    gates = jnp.concatenate(
        [gates, jnp.zeros((2 * heads, LANES - rows), F32)], axis=1
    )
    gates = jnp.concatenate(
        [gates, jnp.zeros((LANES - 2 * heads, LANES), F32)], axis=0
    ).T[:rows]
    scales = []
    for h in range(heads):
        q = queries[:, h * dk : (h + 1) * dk]
        k = keys[:, h * dk : (h + 1) * dk]
        v = values[:, h * dv : (h + 1) * dv]
        f = jnp.broadcast_to(gates[:, h : h + 1], (rows, dv))
        enter = gates[:, heads + h : heads + h + 1]
        iv = enter * v
        nn = f * state_n[:, h, :] + enter * k
        new_n[:, h, :] = nn
        denom = jnp.sum(q * nn, axis=-1, keepdims=True)
        scales.append(jnp.maximum(jnp.abs(denom), 1.0))
        pad = jnp.zeros((LANES - rows, dk), F32)
        q_t = jnp.concatenate([q, pad], axis=0).T
        k_t = jnp.concatenate([k, pad], axis=0).T
        key_cols[h] = k_t
        value_rows[h] = iv
        forget_rows[h] = f
        for t in range(rows):
            c = f[t : t + 1] * state_c[t, h] + k_t[:, t : t + 1] * iv[t : t + 1]
            numer[t : t + 1, h * dv : (h + 1) * dv] = jnp.sum(
                q_t[:, t : t + 1] * c, axis=0, keepdims=True
            )
    head_out = jnp.concatenate(
        [numer[:, h * dv : (h + 1) * dv] / scales[h] for h in range(heads)], axis=1
    ).astype(BF16)
    copies[10].wait()
    part[...] = dot(head_out, w_mixer[...]).astype(BF16)


VMEM = pl.BlockSpec(memory_space=pltpu.VMEM)
HBM = pl.BlockSpec(memory_space=pltpu.HBM)
SMEM = pl.BlockSpec(memory_space=pltpu.SMEM)


def call(body, name, flops, limit, outs, args, scratch=(), specs=None):
    if specs:
        args = [
            pltpu.with_memory_space_constraint(a, pltpu.HBM) if spec is HBM else a
            for a, spec in zip(args, specs)
        ]
    return pl.pallas_call(
        body,
        out_shape=tuple(jax.ShapeDtypeStruct(*o) for o in outs),
        in_specs=specs or [VMEM] * len(args),
        out_specs=tuple([VMEM] * len(outs)),
        scratch_shapes=list(scratch),
        compiler_params=pltpu.CompilerParams(vmem_limit_bytes=limit << 20),
        cost_estimate=pl.CostEstimate(flops=flops, bytes_accessed=flops, transcendentals=0),
        name=name,
    )(*args)


def landing(arrays):
    return [pltpu.VMEM(a.shape, a.dtype) for a in arrays]


def cell(bias_in, bias_forget, *arrays):
    tokens = arrays[0]
    state_m, state_n, state_c = arrays[4], arrays[8], arrays[9]
    rows, width = tokens.shape
    heads, dk, dv = state_c.shape[1:]
    return call(
        cell_kernel,
        "cell",
        1 << 24,
        24,
        (
            ((rows, width), BF16),
            (state_n.shape, F32),
            (state_m.shape, F32),
            ((heads, dk, LANES), F32),
            ((heads, rows, dv), F32),
            ((heads, rows, dv), F32),
        ),
        (bias_in, bias_forget) + arrays,
        landing(arrays)
        + [pltpu.VMEM((rows, heads * dv), F32), pltpu.SemaphoreType.DMA((len(arrays),))],
        [SMEM] * 2 + [HBM] * len(arrays),
    )


def state_kernel(state_c, key_cols, value_rows, forget_rows, new_c):
    rows, heads = state_c.shape[:2]
    for h in range(heads):
        k_t = key_cols[h]
        for t in range(rows):
            new_c[t, h] = (
                forget_rows[h, t : t + 1] * state_c[t, h]
                + k_t[:, t : t + 1] * value_rows[h, t : t + 1]
            )


def prep_kernel(part, tokens, gain, extra, *refs):
    received, (near, mine) = refs[:-2], refs[-2:]
    width = tokens.shape[1]
    cols = mine.shape[1]
    total = part[...].astype(F32)
    for r in received:
        total = total + r[...].astype(F32)
    residual = tokens[...].astype(F32) + total.astype(BF16).astype(F32)
    scaled = residual * lax.rsqrt(
        jnp.mean(residual * residual, axis=-1, keepdims=True) + EPSILON
    )
    near[:, :width] = (scaled * gain[...]).astype(BF16)
    near[:, width:] = extra[...]
    picked = residual[:, :cols]
    for g in range(1, width // cols):
        picked = jnp.where(
            lax.axis_index("tp") == g, residual[:, g * cols : (g + 1) * cols], picked
        )
    mine[...] = picked


def dense_kernel(packed, w_branch, *refs):
    sources, out, targets, sems = refs[:3], refs[3], refs[4:7], refs[7]
    copies = fetch(sources, targets, sems)
    w_gate, w_up, w_down = targets
    width = w_branch.shape[1]
    tp, _, cols = out.shape
    rows = packed[:, :width]
    branch = jax.nn.sigmoid(
        jnp.sum(rows.astype(F32) * w_branch[...], axis=1, keepdims=True)
    )
    copies[0].wait()
    gate = dot(rows, w_gate[...])
    copies[1].wait()
    hidden = (gate * jax.nn.sigmoid(gate) * dot(rows, w_up[...])).astype(BF16)
    copies[2].wait()
    for h in range(tp):
        at = pl.multiple_of((lax.axis_index("tp") ^ h) * cols, LANES)
        out[h] = branch * dot(hidden, w_down[:, pl.ds(at, cols)])


def expert_kernel(top, near, far, w_gate, w_up, w_down, *refs):
    send, keep = refs[-2:]
    half = near.shape[0]
    width = w_gate.shape[0]
    tp, _, cols = keep.shape
    packed = jnp.concatenate([far[...], near[...]], axis=0)
    rows = packed[:, :width]
    extra = packed[:, width:].astype(F32)
    own = lax.axis_index("ep").astype(F32)
    lane = lax.broadcasted_iota(jnp.int32, extra.shape, 1)
    scale = pltpu.roll(extra, LANES // 2, 1)
    valid = lane < top
    total = jnp.sum(jnp.where(valid, scale, 0.0), axis=1, keepdims=True)
    mine = jnp.sum(jnp.where(valid & (extra == own), scale, 0.0), axis=1, keepdims=True)
    weight = mine / total
    gate = jnp.minimum(dot(rows, w_gate[...]), CLAMP_LIMIT)
    up = jnp.clip(dot(rows, w_up[...]), -CLAMP_LIMIT, CLAMP_LIMIT)
    hidden = (gate * jax.nn.sigmoid(SWISH_ALPHA * gate) * (up + 1.0)).astype(BF16)
    for h in range(tp):
        at = pl.multiple_of((lax.axis_index("tp") ^ h) * cols, LANES)
        piece = dot(hidden, w_down[:, pl.ds(at, cols)]) * weight
        send[h] = piece[:half].astype(BF16)
        keep[h] = piece[half:]
        if refs[:-2]:
            dense = refs[0]
            keep[h, : dense.shape[1]] += dense[h]


def experts(name, top, tp, near, far, *weights):
    half = near.shape[0]
    cols = weights[2].shape[1] // tp
    return call(
        functools.partial(expert_kernel, top),
        name,
        1 << 26,
        24,
        (((tp, half, cols), BF16), ((tp, half, cols), F32)),
        (near, far) + weights,
    )


def bits_of(size):
    return [1 << b for b in range(size.bit_length() - 1)]


def combos(bits):
    masks = [0]
    for bit in bits:
        masks = masks + [m ^ bit for m in masks]
    return masks


def hop(x, ep_mask, tp_mask):
    ep, tp = lax.axis_size("ep"), lax.axis_size("tp")
    pairs = [
        (e * tp + t, (e ^ ep_mask) * tp + (t ^ tp_mask)) for e in range(ep) for t in range(tp)
    ]
    return lax.ppermute(x, AXES, pairs)


def local(
    tokens,
    norm_gain,
    w_query,
    w_key,
    w_value,
    w_input_gate,
    w_forget_gate,
    input_bias,
    forget_bias,
    state_c,
    state_n,
    state_m,
    w_mixer_out,
    ffn_gain,
    routes,
    route_scale,
    w_expert_gate,
    w_expert_up,
    w_expert_down,
    w_dense_gate,
    w_dense_up,
    w_dense_down,
    w_branch_gate,
):
    count, width = tokens.shape
    top = routes.shape[1]
    tp, ep = lax.axis_size("tp"), lax.axis_size("ep")
    cols = width // tp
    part, new_n, new_m, key_cols, value_rows, forget_rows = cell(
        input_bias,
        forget_bias,
        tokens,
        norm_gain.reshape(1, width),
        w_input_gate.T,
        w_forget_gate.T,
        state_m.T,
        w_query,
        w_key,
        w_value,
        state_n,
        state_c,
        w_mixer_out,
    )
    tp_masks = combos(bits_of(tp))
    received = [hop(part, 0, mask) for mask in tp_masks[1:]]
    (new_c,) = call(
        state_kernel,
        "state",
        1 << 23,
        16,
        ((state_c.shape, F32),),
        (state_c, key_cols, value_rows, forget_rows),
    )
    blank = jnp.zeros((count, LANES // 2 - top), BF16)
    extra = jnp.concatenate([routes.astype(BF16), blank, route_scale, blank], axis=1)
    near, residual = call(
        prep_kernel,
        "prep",
        1 << 20,
        16,
        (((count, width + LANES), BF16), ((count, cols), F32)),
        [part, tokens, ffn_gain.reshape(1, width), extra] + received,
    )
    matrices = (w_dense_gate, w_dense_up, w_dense_down)
    (dense,) = call(
        dense_kernel,
        "dense",
        1 << 23,
        16,
        (((tp, count, cols), F32),),
        (near, w_branch_gate.astype(F32).reshape(1, width)) + matrices,
        landing(matrices) + [pltpu.SemaphoreType.DMA((len(matrices),))],
        [VMEM] * 2 + [HBM] * 3,
    )
    rest = [bit ^ 1 for bit in bits_of(ep)[1:]]
    x_bits = rest[: len(rest) % 2 or 2]
    groups = [combos(rest[i : i + 2]) for i in range(len(x_bits), len(rest), 2)]
    for masks in reversed(groups):
        near = jnp.concatenate([near] + [hop(near, m, 0) for m in masks[1:]], axis=0)
    x_masks = combos(x_bits)
    others = [hop(near, m, 0) for m in x_masks[1:]]
    far = hop(near, 1, 0)
    weights = (w_expert_gate[0], w_expert_up[0], w_expert_down[0])
    send, keep = experts("near_rows", top, tp, near, far, *weights, dense)
    sums = [keep + hop(send, 1, 0).astype(F32)]
    for rows in others:
        send, keep = experts("far_rows", top, tp, rows, hop(rows, 1, 0), *weights)
        sums.append(keep + hop(send, 1, 0).astype(F32))
    total = sums[0][0]
    for i, a in enumerate(x_masks):
        for j, b in enumerate(tp_masks):
            if i or j:
                total = total + hop(sums[i][j].astype(BF16), a, b).astype(F32)
    for masks in groups:
        size = total.shape[0] // len(masks)
        kept = total[:size]
        for i, m in enumerate(masks[1:], 1):
            piece = total[i * size : (i + 1) * size].astype(BF16)
            kept = kept + hop(piece, m, 0).astype(F32)
        total = kept
    output = (residual + total).astype(BF16)
    new_m = new_m.T
    return (output, new_c, new_n, new_m)


def solution(mesh):
    in_specs = (
        P("ep", None),
        P(),
        P(None, "tp"),
        P(None, "tp"),
        P(None, "tp"),
        P(),
        P(),
        P(),
        P(),
        P("ep", "tp", None, None),
        P("ep", "tp", None),
        P("ep", "tp"),
        P("tp", None),
        P(),
        P("ep", None),
        P("ep", None),
        P("ep", None, "tp"),
        P("ep", None, "tp"),
        P("ep", "tp", None),
        P(None, "tp"),
        P(None, "tp"),
        P("tp", None),
        P(),
    )
    out_specs = (P("ep", "tp"), P("ep", "tp", None, None), P("ep", "tp", None), P("ep", "tp"))
    return jax.shard_map(local, mesh=mesh, in_specs=in_specs, out_specs=out_specs, check_vma=False)
```

```python
import functools
import jax
import jax.numpy as jnp
from jax import lax
from jax.experimental import pallas as pl
from jax.experimental.pallas import tpu as pltpu
from jax.sharding import PartitionSpec as P

EPSILON = 1e-06
CLAMP_LIMIT = 7.0
SWISH_ALPHA = 1.702
AXES = ("ep", "tp")
LANES = 128
F32 = jnp.float32
BF16 = jnp.bfloat16


def dot(a, b):
    return jnp.dot(a, b, preferred_element_type=F32)


def across(a, b):
    return lax.dot_general(a, b, (((1,), (1,)), ((), ())), preferred_element_type=F32)


def own_rows(both, heads):
    mine = both[:heads]
    for g in range(1, both.shape[0] // heads):
        mine = jnp.where(
            lax.axis_index("tp") == g, both[g * heads : (g + 1) * heads], mine
        )
    return mine


def bias_rows(bias, heads, rows):
    first = lax.axis_index("tp") * heads
    at = lax.broadcasted_iota(jnp.int32, (heads, rows), 0)
    out = jnp.full((heads, rows), bias[first], F32)
    for h in range(1, heads):
        out = jnp.where(at == h, bias[first + h], out)
    return out


def fetch(sources, targets, sems):
    copies = [
        pltpu.make_async_copy(a, b, sems.at[i])
        for i, (a, b) in enumerate(zip(sources, targets))
    ]
    for copy in copies:
        copy.start()
    return copies


def cell_kernel(*refs):
    count = (len(refs) - 8) // 2
    sources = refs[:count]
    part, new_n, new_m, key_cols, value_rows, forget_rows = refs[count : count + 6]
    targets = refs[count + 6 : 2 * count + 6]
    numer, sems = refs[2 * count + 6 :]
    (
        tokens,
        gain,
        w_query,
        w_key,
        w_value,
        bias_in,
        bias_forget,
        w_in,
        w_forget,
        state_m,
        state_n,
        w_mixer,
        state_c,
    ) = targets
    copies = fetch(sources, targets, sems)
    rows = tokens.shape[0]
    heads, dk, dv = state_c.shape[1:]
    for copy in copies[:2]:
        copy.wait()
    x = tokens[...].astype(F32)
    normed = x * lax.rsqrt(jnp.mean(x * x, axis=-1, keepdims=True) + EPSILON)
    normed = (normed * gain[...]).astype(BF16)
    copies[2].wait()
    queries = dot(normed, w_query[...]).astype(BF16).astype(F32)
    copies[3].wait()
    keys = dot(normed, w_key[...]).astype(BF16).astype(F32) * dk ** (-0.5)
    copies[4].wait()
    values = dot(normed, w_value[...]).astype(BF16).astype(F32)
    for copy in copies[5:-2]:
        copy.wait()
    in_pre = own_rows(across(w_in[...], normed), heads) + bias_rows(bias_in, heads, rows)
    forget_pre = own_rows(across(w_forget[...], normed), heads) + bias_rows(
        bias_forget, heads, rows
    )
    forget_log = jnp.minimum(forget_pre, 0.0) - jnp.log1p(jnp.exp(-jnp.abs(forget_pre)))
    carried = forget_log + state_m[...]
    top = jnp.maximum(carried, in_pre)
    new_m[...] = top
    gates = jnp.concatenate([jnp.exp(carried - top), jnp.exp(in_pre - top)], axis=0)
    gates = jnp.concatenate(
        [gates, jnp.zeros((2 * heads, LANES - rows), F32)], axis=1
    )
    gates = jnp.concatenate(
        [gates, jnp.zeros((LANES - 2 * heads, LANES), F32)], axis=0
    ).T[:rows]
    scales, columns = [], []
    for h in range(heads):
        q = queries[:, h * dk : (h + 1) * dk]
        k = keys[:, h * dk : (h + 1) * dk]
        v = values[:, h * dv : (h + 1) * dv]
        f = jnp.broadcast_to(gates[:, h : h + 1], (rows, dv))
        enter = gates[:, heads + h : heads + h + 1]
        iv = enter * v
        nn = f * state_n[:, h, :] + enter * k
        new_n[:, h, :] = nn
        denom = jnp.sum(q * nn, axis=-1, keepdims=True)
        scales.append(jnp.maximum(jnp.abs(denom), 1.0))
        pad = jnp.zeros((LANES - rows, dk), F32)
        q_t = jnp.concatenate([q, pad], axis=0).T
        k_t = jnp.concatenate([k, pad], axis=0).T
        key_cols[h] = k_t
        value_rows[h] = iv
        forget_rows[h] = f
        gain_qk = jnp.sum(q * k, axis=-1, keepdims=True)
        columns.append((f, gain_qk * iv, q_t))
    copies[-1].wait()
    for t in range(rows):
        for h in range(heads):
            numer[t : t + 1, h * dv : (h + 1) * dv] = jnp.sum(
                columns[h][2][:, t : t + 1] * state_c[t, h], axis=0, keepdims=True
            )
    head_out = jnp.concatenate(
        [
            (f * numer[:, h * dv : (h + 1) * dv] + w) / scales[h]
            for h, (f, w, _) in enumerate(columns)
        ],
        axis=1,
    ).astype(BF16)
    copies[-2].wait()
    part[...] = dot(head_out, w_mixer[...]).astype(BF16)


VMEM = pl.BlockSpec(memory_space=pltpu.VMEM)
HBM = pl.BlockSpec(memory_space=pltpu.HBM)
SMEM = pl.BlockSpec(memory_space=pltpu.SMEM)


def call(body, name, flops, limit, outs, args, scratch=(), specs=None):
    if specs:
        args = [
            pltpu.with_memory_space_constraint(a, pltpu.HBM) if spec is HBM else a
            for a, spec in zip(args, specs)
        ]
    return pl.pallas_call(
        body,
        out_shape=tuple(jax.ShapeDtypeStruct(*o) for o in outs),
        in_specs=specs or [VMEM] * len(args),
        out_specs=tuple([VMEM] * len(outs)),
        scratch_shapes=list(scratch),
        compiler_params=pltpu.CompilerParams(vmem_limit_bytes=limit << 20),
        cost_estimate=pl.CostEstimate(flops=flops, bytes_accessed=flops, transcendentals=0),
        name=name,
    )(*args)


def landing(arrays):
    return [pltpu.VMEM(a.shape, a.dtype) for a in arrays]


def cell(*arrays):
    tokens = arrays[0]
    state_m, state_n, state_c = arrays[9], arrays[10], arrays[12]
    rows, width = tokens.shape
    heads, dk, dv = state_c.shape[1:]
    spaces = [pltpu.SMEM if a.ndim == 1 else pltpu.VMEM for a in arrays]
    return call(
        cell_kernel,
        "cell",
        1 << 24,
        24,
        (
            ((rows, width), BF16),
            (state_n.shape, F32),
            (state_m.shape, F32),
            ((heads, dk, LANES), F32),
            ((heads, rows, dv), F32),
            ((heads, rows, dv), F32),
        ),
        arrays,
        [space(a.shape, a.dtype) for space, a in zip(spaces, arrays)]
        + [
            pltpu.VMEM((rows, heads * dv), F32),
            pltpu.SemaphoreType.DMA((len(arrays),)),
        ],
        [HBM] * len(arrays),
    )


def state_kernel(state_c, key_cols, value_rows, forget_rows, new_c):
    rows, heads = state_c.shape[:2]
    for h in range(heads):
        k_t = key_cols[h]
        for t in range(rows):
            new_c[t, h] = (
                forget_rows[h, t : t + 1] * state_c[t, h]
                + k_t[:, t : t + 1] * value_rows[h, t : t + 1]
            )


def prep_kernel(part, tokens, gain, extra, *refs):
    received, (near, mine) = refs[:-2], refs[-2:]
    width = tokens.shape[1]
    cols = mine.shape[1]
    total = part[...].astype(F32)
    for r in received:
        total = total + r[...].astype(F32)
    residual = tokens[...].astype(F32) + total.astype(BF16).astype(F32)
    scaled = residual * lax.rsqrt(
        jnp.mean(residual * residual, axis=-1, keepdims=True) + EPSILON
    )
    near[:, :width] = (scaled * gain[...]).astype(BF16)
    near[:, width:] = extra[...]
    picked = residual[:, :cols]
    for g in range(1, width // cols):
        picked = jnp.where(
            lax.axis_index("tp") == g, residual[:, g * cols : (g + 1) * cols], picked
        )
    mine[...] = picked


def dense_kernel(packed, w_branch, *refs):
    sources, out, targets, sems = refs[:3], refs[3], refs[4:7], refs[7]
    copies = fetch(sources, targets, sems)
    w_gate, w_up, w_down = targets
    width = w_branch.shape[1]
    tp, _, cols = out.shape
    rows = packed[:, :width]
    branch = jax.nn.sigmoid(
        jnp.sum(rows.astype(F32) * w_branch[...], axis=1, keepdims=True)
    )
    copies[0].wait()
    gate = dot(rows, w_gate[...])
    copies[1].wait()
    hidden = (gate * jax.nn.sigmoid(gate) * dot(rows, w_up[...])).astype(BF16)
    copies[2].wait()
    for h in range(tp):
        at = pl.multiple_of((lax.axis_index("tp") ^ h) * cols, LANES)
        out[h] = branch * dot(hidden, w_down[:, pl.ds(at, cols)])


def expert_kernel(top, near, far, w_gate, w_up, w_down, *refs):
    send, keep = refs[-2:]
    half = near.shape[0]
    width = w_gate.shape[0]
    tp, _, cols = keep.shape
    packed = jnp.concatenate([far[...], near[...]], axis=0)
    rows = packed[:, :width]
    extra = packed[:, width:].astype(F32)
    own = lax.axis_index("ep").astype(F32)
    lane = lax.broadcasted_iota(jnp.int32, extra.shape, 1)
    scale = pltpu.roll(extra, LANES // 2, 1)
    valid = lane < top
    total = jnp.sum(jnp.where(valid, scale, 0.0), axis=1, keepdims=True)
    mine = jnp.sum(jnp.where(valid & (extra == own), scale, 0.0), axis=1, keepdims=True)
    weight = mine / total
    gate = jnp.minimum(dot(rows, w_gate[...]), CLAMP_LIMIT)
    up = jnp.clip(dot(rows, w_up[...]), -CLAMP_LIMIT, CLAMP_LIMIT)
    hidden = (gate * jax.nn.sigmoid(SWISH_ALPHA * gate) * (up + 1.0)).astype(BF16)
    for h in range(tp):
        at = pl.multiple_of((lax.axis_index("tp") ^ h) * cols, LANES)
        piece = dot(hidden, w_down[:, pl.ds(at, cols)]) * weight
        send[h] = piece[:half].astype(BF16)
        keep[h] = piece[half:]
        if refs[:-2]:
            dense = refs[0]
            keep[h, : dense.shape[1]] += dense[h]


def experts(name, top, tp, near, far, *weights):
    half = near.shape[0]
    cols = weights[2].shape[1] // tp
    return call(
        functools.partial(expert_kernel, top),
        name,
        1 << 26,
        24,
        (((tp, half, cols), BF16), ((tp, half, cols), F32)),
        (near, far) + weights,
    )


def bits_of(size):
    return [1 << b for b in range(size.bit_length() - 1)]


def combos(bits):
    masks = [0]
    for bit in bits:
        masks = masks + [m ^ bit for m in masks]
    return masks


def hop(x, ep_mask, tp_mask):
    ep, tp = lax.axis_size("ep"), lax.axis_size("tp")
    pairs = [
        (e * tp + t, (e ^ ep_mask) * tp + (t ^ tp_mask)) for e in range(ep) for t in range(tp)
    ]
    return lax.ppermute(x, AXES, pairs)


def local(
    tokens,
    norm_gain,
    w_query,
    w_key,
    w_value,
    w_input_gate,
    w_forget_gate,
    input_bias,
    forget_bias,
    state_c,
    state_n,
    state_m,
    w_mixer_out,
    ffn_gain,
    routes,
    route_scale,
    w_expert_gate,
    w_expert_up,
    w_expert_down,
    w_dense_gate,
    w_dense_up,
    w_dense_down,
    w_branch_gate,
):
    count, width = tokens.shape
    top = routes.shape[1]
    tp, ep = lax.axis_size("tp"), lax.axis_size("ep")
    cols = width // tp
    part, new_n, new_m, key_cols, value_rows, forget_rows = cell(
        tokens,
        norm_gain.reshape(1, width),
        w_query,
        w_key,
        w_value,
        input_bias,
        forget_bias,
        w_input_gate.T,
        w_forget_gate.T,
        state_m.T,
        state_n,
        w_mixer_out,
        state_c,
    )
    tp_masks = combos(bits_of(tp))
    received = [hop(part, 0, mask) for mask in tp_masks[1:]]
    (new_c,) = call(
        state_kernel,
        "state",
        1 << 23,
        16,
        ((state_c.shape, F32),),
        (state_c, key_cols, value_rows, forget_rows),
    )
    blank = jnp.zeros((count, LANES // 2 - top), BF16)
    extra = jnp.concatenate([routes.astype(BF16), blank, route_scale, blank], axis=1)
    near, residual = call(
        prep_kernel,
        "prep",
        1 << 20,
        16,
        (((count, width + LANES), BF16), ((count, cols), F32)),
        [part, tokens, ffn_gain.reshape(1, width), extra] + received,
    )
    matrices = (w_dense_gate, w_dense_up, w_dense_down)
    (dense,) = call(
        dense_kernel,
        "dense",
        1 << 23,
        16,
        (((tp, count, cols), F32),),
        (near, w_branch_gate.astype(F32).reshape(1, width)) + matrices,
        landing(matrices) + [pltpu.SemaphoreType.DMA((len(matrices),))],
        [VMEM] * 2 + [HBM] * 3,
    )
    rest = [bit ^ 1 for bit in bits_of(ep)[1:]]
    x_bits = rest[: len(rest) % 2 or 2]
    groups = [combos(rest[i : i + 2]) for i in range(len(x_bits), len(rest), 2)]
    groups = [m[:2] + m[:1:-1] for m in groups]
    for masks in reversed(groups):
        near = jnp.concatenate([near] + [hop(near, m, 0) for m in masks[1:]], axis=0)
    x_masks = combos(x_bits)
    others = [hop(near, m, 0) for m in x_masks[1:]]
    far = hop(near, 1, 0)
    weights = (w_expert_gate[0], w_expert_up[0], w_expert_down[0])
    send, keep = experts("near_rows", top, tp, near, far, *weights, dense)
    sums = [keep + hop(send, 1, 0).astype(F32)]
    for rows in others:
        send, keep = experts("far_rows", top, tp, rows, hop(rows, 1, 0), *weights)
        sums.append(keep + hop(send, 1, 0).astype(F32))
    total = sums[0][0]
    for i, a in enumerate(x_masks):
        for j, b in enumerate(tp_masks):
            if i or j:
                total = total + hop(sums[i][j].astype(BF16), a, b).astype(F32)
    for masks in groups:
        size = total.shape[0] // len(masks)
        kept = total[:size]
        for i in (2, 3, 1):
            piece = total[i * size : (i + 1) * size].astype(BF16)
            kept = kept + hop(piece, masks[i], 0).astype(F32)
        total = kept
    output = (residual + total).astype(BF16)
    new_m = new_m.T
    return (output, new_c, new_n, new_m)


def solution(mesh):
    in_specs = (
        P("ep", None),
        P(),
        P(None, "tp"),
        P(None, "tp"),
        P(None, "tp"),
        P(),
        P(),
        P(),
        P(),
        P("ep", "tp", None, None),
        P("ep", "tp", None),
        P("ep", "tp"),
        P("tp", None),
        P(),
        P("ep", None),
        P("ep", None),
        P("ep", None, "tp"),
        P("ep", None, "tp"),
        P("ep", "tp", None),
        P(None, "tp"),
        P(None, "tp"),
        P("tp", None),
        P(),
    )
    out_specs = (P("ep", "tp"), P("ep", "tp", None, None), P("ep", "tp", None), P("ep", "tp"))
    return jax.shard_map(local, mesh=mesh, in_specs=in_specs, out_specs=out_specs, check_vma=False)
```

```python
import functools
import jax
import jax.numpy as jnp
from jax import lax
from jax.experimental import pallas as pl
from jax.experimental.pallas import tpu as pltpu
from jax.sharding import PartitionSpec as P

EPSILON = 1e-06
CLAMP_LIMIT = 7.0
SWISH_ALPHA = 1.702
AXES = ("ep", "tp")
LANES = 128
F32 = jnp.float32
BF16 = jnp.bfloat16


def dot(a, b):
    return jnp.dot(a, b, preferred_element_type=F32)


def across(a, b):
    return lax.dot_general(a, b, (((1,), (1,)), ((), ())), preferred_element_type=F32)


def own_rows(both, heads):
    mine = both[:heads]
    for g in range(1, both.shape[0] // heads):
        mine = jnp.where(
            lax.axis_index("tp") == g, both[g * heads : (g + 1) * heads], mine
        )
    return mine


def bias_rows(bias, heads, rows):
    first = lax.axis_index("tp") * heads
    at = lax.broadcasted_iota(jnp.int32, (heads, rows), 0)
    out = jnp.full((heads, rows), bias[first], F32)
    for h in range(1, heads):
        out = jnp.where(at == h, bias[first + h], out)
    return out


def fetch(sources, targets, sems):
    copies = [
        pltpu.make_async_copy(a, b, sems.at[i])
        for i, (a, b) in enumerate(zip(sources, targets))
    ]
    for copy in copies:
        copy.start()
    return copies


def cell_kernel(*refs):
    count = (len(refs) - 8) // 2
    sources = refs[:count]
    part, new_n, new_m, key_cols, value_rows, forget_rows = refs[count : count + 6]
    targets = refs[count + 6 : 2 * count + 6]
    numer, sems = refs[2 * count + 6 :]
    (
        tokens,
        gain,
        w_query,
        w_key,
        w_value,
        bias_in,
        bias_forget,
        w_in,
        w_forget,
        state_m,
        state_n,
        w_mixer,
        state_c,
    ) = targets
    order = (0, 1, 5, 6, 7, 8, 9, 2, 3, 4, 10, 11, 12)
    started = fetch([sources[i] for i in order], [targets[i] for i in order], sems)
    copies = [started[order.index(i)] for i in range(count)]
    rows = tokens.shape[0]
    heads, dk, dv = state_c.shape[1:]
    for copy in copies[:2]:
        copy.wait()
    x = tokens[...].astype(F32)
    normed = x * lax.rsqrt(jnp.mean(x * x, axis=-1, keepdims=True) + EPSILON)
    normed = (normed * gain[...]).astype(BF16)
    for copy in copies[5:-3]:
        copy.wait()
    in_pre = own_rows(across(w_in[...], normed), heads) + bias_rows(bias_in, heads, rows)
    forget_pre = own_rows(across(w_forget[...], normed), heads) + bias_rows(
        bias_forget, heads, rows
    )
    forget_log = jnp.minimum(forget_pre, 0.0) - jnp.log1p(jnp.exp(-jnp.abs(forget_pre)))
    carried = forget_log + state_m[...]
    top = jnp.maximum(carried, in_pre)
    new_m[...] = top
    gates = jnp.concatenate([jnp.exp(carried - top), jnp.exp(in_pre - top)], axis=0)
    gates = jnp.concatenate(
        [gates, jnp.zeros((2 * heads, LANES - rows), F32)], axis=1
    )
    gates = jnp.concatenate(
        [gates, jnp.zeros((LANES - 2 * heads, LANES), F32)], axis=0
    ).T[:rows]
    copies[2].wait()
    queries = dot(normed, w_query[...]).astype(BF16).astype(F32)
    copies[3].wait()
    keys = dot(normed, w_key[...]).astype(BF16).astype(F32) * dk ** (-0.5)
    copies[4].wait()
    values = dot(normed, w_value[...]).astype(BF16).astype(F32)
    copies[-3].wait()
    scales, columns = [], []
    for h in range(heads):
        q = queries[:, h * dk : (h + 1) * dk]
        k = keys[:, h * dk : (h + 1) * dk]
        v = values[:, h * dv : (h + 1) * dv]
        f = jnp.broadcast_to(gates[:, h : h + 1], (rows, dv))
        enter = gates[:, heads + h : heads + h + 1]
        iv = enter * v
        nn = f * state_n[:, h, :] + enter * k
        new_n[:, h, :] = nn
        denom = jnp.sum(q * nn, axis=-1, keepdims=True)
        scales.append(jnp.maximum(jnp.abs(denom), 1.0))
        pad = jnp.zeros((LANES - rows, dk), F32)
        q_t = jnp.concatenate([q, pad], axis=0).T
        k_t = jnp.concatenate([k, pad], axis=0).T
        key_cols[h] = k_t
        value_rows[h] = iv
        forget_rows[h] = f
        gain_qk = jnp.sum(q * k, axis=-1, keepdims=True)
        columns.append((f, gain_qk * iv, q_t))
    copies[-1].wait()
    for t in range(rows):
        for h in range(heads):
            numer[t : t + 1, h * dv : (h + 1) * dv] = jnp.sum(
                columns[h][2][:, t : t + 1] * state_c[t, h], axis=0, keepdims=True
            )
    head_out = jnp.concatenate(
        [
            (f * numer[:, h * dv : (h + 1) * dv] + w) / scales[h]
            for h, (f, w, _) in enumerate(columns)
        ],
        axis=1,
    ).astype(BF16)
    copies[-2].wait()
    part[...] = dot(head_out, w_mixer[...]).astype(BF16)


VMEM = pl.BlockSpec(memory_space=pltpu.VMEM)
HBM = pl.BlockSpec(memory_space=pltpu.HBM)
SMEM = pl.BlockSpec(memory_space=pltpu.SMEM)


def call(body, flops, limit, outs, args, scratch=(), specs=None):
    if specs:
        args = [
            pltpu.with_memory_space_constraint(a, pltpu.HBM) if spec is HBM else a
            for a, spec in zip(args, specs)
        ]
    return pl.pallas_call(
        body,
        out_shape=tuple(jax.ShapeDtypeStruct(*o) for o in outs),
        in_specs=specs or [VMEM] * len(args),
        out_specs=tuple([VMEM] * len(outs)),
        scratch_shapes=list(scratch),
        compiler_params=pltpu.CompilerParams(vmem_limit_bytes=limit << 20),
        cost_estimate=pl.CostEstimate(flops=flops, bytes_accessed=flops, transcendentals=0),
    )(*args)


def landing(arrays):
    return [pltpu.VMEM(a.shape, a.dtype) for a in arrays]


def cell(*arrays):
    tokens = arrays[0]
    state_m, state_n, state_c = arrays[9], arrays[10], arrays[12]
    rows, width = tokens.shape
    heads, dk, dv = state_c.shape[1:]
    spaces = [pltpu.SMEM if a.ndim == 1 else pltpu.VMEM for a in arrays]
    return call(
        cell_kernel,
        1 << 24,
        24,
        (
            ((rows, width), BF16),
            (state_n.shape, F32),
            (state_m.shape, F32),
            ((heads, dk, LANES), F32),
            ((heads, rows, dv), F32),
            ((heads, rows, dv), F32),
        ),
        arrays,
        [space(a.shape, a.dtype) for space, a in zip(spaces, arrays)]
        + [
            pltpu.VMEM((rows, heads * dv), F32),
            pltpu.SemaphoreType.DMA((len(arrays),)),
        ],
        [HBM] * len(arrays),
    )


def state_kernel(state_c, key_cols, value_rows, forget_rows, new_c):
    rows, heads = state_c.shape[:2]
    for h in range(heads):
        k_t = key_cols[h]
        for t in range(rows):
            new_c[t, h] = (
                forget_rows[h, t : t + 1] * state_c[t, h]
                + k_t[:, t : t + 1] * value_rows[h, t : t + 1]
            )


def prep_kernel(part, tokens, gain, extra, *refs):
    received, (near, mine) = refs[:-2], refs[-2:]
    width = tokens.shape[1]
    cols = mine.shape[1]
    total = part[...].astype(F32)
    for r in received:
        total = total + r[...].astype(F32)
    residual = tokens[...].astype(F32) + total.astype(BF16).astype(F32)
    scaled = residual * lax.rsqrt(
        jnp.mean(residual * residual, axis=-1, keepdims=True) + EPSILON
    )
    near[:, :width] = (scaled * gain[...]).astype(BF16)
    near[:, width:] = extra[...]
    picked = residual[:, :cols]
    for g in range(1, width // cols):
        picked = jnp.where(
            lax.axis_index("tp") == g, residual[:, g * cols : (g + 1) * cols], picked
        )
    mine[...] = picked


def dense_kernel(packed, w_branch, *refs):
    sources, out, targets, sems = refs[:3], refs[3], refs[4:7], refs[7]
    copies = fetch(sources, targets, sems)
    w_gate, w_up, w_down = targets
    width = w_branch.shape[1]
    tp, _, cols = out.shape
    rows = packed[:, :width]
    branch = jax.nn.sigmoid(
        jnp.sum(rows.astype(F32) * w_branch[...], axis=1, keepdims=True)
    )
    copies[0].wait()
    gate = dot(rows, w_gate[...])
    copies[1].wait()
    hidden = (gate * jax.nn.sigmoid(gate) * dot(rows, w_up[...])).astype(BF16)
    copies[2].wait()
    for h in range(tp):
        at = pl.multiple_of((lax.axis_index("tp") ^ h) * cols, LANES)
        out[h] = branch * dot(hidden, w_down[:, pl.ds(at, cols)])


def expert_kernel(top, near, far, w_gate, w_up, w_down, *refs):
    send, keep = refs[-2:]
    half = near.shape[0]
    width = w_gate.shape[0]
    tp, _, cols = keep.shape
    packed = jnp.concatenate([far[...], near[...]], axis=0)
    rows = packed[:, :width]
    extra = packed[:, width:].astype(F32)
    own = lax.axis_index("ep").astype(F32)
    lane = lax.broadcasted_iota(jnp.int32, extra.shape, 1)
    scale = pltpu.roll(extra, LANES // 2, 1)
    valid = lane < top
    total = jnp.sum(jnp.where(valid, scale, 0.0), axis=1, keepdims=True)
    mine = jnp.sum(jnp.where(valid & (extra == own), scale, 0.0), axis=1, keepdims=True)
    weight = mine / total
    gate = jnp.minimum(dot(rows, w_gate[...]), CLAMP_LIMIT)
    up = jnp.clip(dot(rows, w_up[...]), -CLAMP_LIMIT, CLAMP_LIMIT)
    hidden = (gate * jax.nn.sigmoid(SWISH_ALPHA * gate) * (up + 1.0)).astype(BF16)
    for h in range(tp):
        at = pl.multiple_of((lax.axis_index("tp") ^ h) * cols, LANES)
        piece = dot(hidden, w_down[:, pl.ds(at, cols)]) * weight
        send[h] = piece[:half].astype(BF16)
        keep[h] = piece[half:]
        if refs[:-2]:
            dense = refs[0]
            keep[h, : dense.shape[1]] += dense[h]


def experts(top, tp, near, far, *weights):
    half = near.shape[0]
    cols = weights[2].shape[1] // tp
    return call(
        functools.partial(expert_kernel, top),
        1 << 26,
        24,
        (((tp, half, cols), BF16), ((tp, half, cols), F32)),
        (near, far) + weights,
    )


def bits_of(size):
    return [1 << b for b in range(size.bit_length() - 1)]


def combos(bits):
    masks = [0]
    for bit in bits:
        masks = masks + [m ^ bit for m in masks]
    return masks


def hop(x, ep_mask, tp_mask):
    ep, tp = lax.axis_size("ep"), lax.axis_size("tp")
    pairs = [
        (e * tp + t, (e ^ ep_mask) * tp + (t ^ tp_mask)) for e in range(ep) for t in range(tp)
    ]
    return lax.ppermute(x, AXES, pairs)


def local(
    tokens,
    norm_gain,
    w_query,
    w_key,
    w_value,
    w_input_gate,
    w_forget_gate,
    input_bias,
    forget_bias,
    state_c,
    state_n,
    state_m,
    w_mixer_out,
    ffn_gain,
    routes,
    route_scale,
    w_expert_gate,
    w_expert_up,
    w_expert_down,
    w_dense_gate,
    w_dense_up,
    w_dense_down,
    w_branch_gate,
):
    count, width = tokens.shape
    top = routes.shape[1]
    tp, ep = lax.axis_size("tp"), lax.axis_size("ep")
    cols = width // tp
    part, new_n, new_m, key_cols, value_rows, forget_rows = cell(
        tokens,
        norm_gain.reshape(1, width),
        w_query,
        w_key,
        w_value,
        input_bias,
        forget_bias,
        w_input_gate.T,
        w_forget_gate.T,
        state_m.T,
        state_n,
        w_mixer_out,
        state_c,
    )
    tp_masks = combos(bits_of(tp))
    received = [hop(part, 0, mask) for mask in tp_masks[1:]]
    (new_c,) = call(
        state_kernel,
        1 << 23,
        16,
        ((state_c.shape, F32),),
        (state_c, key_cols, value_rows, forget_rows),
    )
    blank = jnp.zeros((count, LANES // 2 - top), BF16)
    extra = jnp.concatenate([routes.astype(BF16), blank, route_scale, blank], axis=1)
    near, residual = call(
        prep_kernel,
        1 << 20,
        16,
        (((count, width + LANES), BF16), ((count, cols), F32)),
        [part, tokens, ffn_gain.reshape(1, width), extra] + received,
    )
    matrices = (w_dense_gate, w_dense_up, w_dense_down)
    (dense,) = call(
        dense_kernel,
        1 << 23,
        16,
        (((tp, count, cols), F32),),
        (near, w_branch_gate.astype(F32).reshape(1, width)) + matrices,
        landing(matrices) + [pltpu.SemaphoreType.DMA((len(matrices),))],
        [VMEM] * 2 + [HBM] * 3,
    )
    rest = [bit ^ 1 for bit in bits_of(ep)[1:]]
    x_bits = rest[: len(rest) % 2 or 2]
    groups = [combos(rest[i : i + 2]) for i in range(len(x_bits), len(rest), 2)]
    groups = [m[:2] + m[:1:-1] for m in groups]
    for masks in reversed(groups):
        near = jnp.concatenate(
            [near] + [hop(near, m, 0) for i, m in enumerate(masks) if i], axis=0
        )
    x_masks = combos(x_bits)
    others = [hop(near, m, 0) for m in x_masks[1:]]
    far = hop(near, 1, 0)
    weights = (w_expert_gate[0], w_expert_up[0], w_expert_down[0])
    send, keep = experts(top, tp, near, far, *weights, dense)
    sums = [keep + hop(send, 1, 0).astype(F32)]
    for rows in others:
        other = hop(rows, 1, 0)
        send, keep = experts(top, tp, rows, other, *weights)
        sums.append(keep + hop(send, 1, 0).astype(F32))
    total = sums[0][0]
    for i, a in enumerate(x_masks):
        for j, b in enumerate(tp_masks):
            if i or j:
                total = total + hop(sums[i][j].astype(BF16), a, b).astype(F32)
    for masks in groups:
        size = total.shape[0] // len(masks)
        kept = total[:size]
        for i in (2, 3, 1):
            piece = total[i * size : (i + 1) * size].astype(BF16)
            kept = kept + hop(piece, masks[i], 0).astype(F32)
        total = kept
    output = (residual + total).astype(BF16)
    new_m = new_m.T
    return (output, new_c, new_n, new_m)


def solution(mesh):
    in_specs = (
        P("ep", None),
        P(),
        P(None, "tp"),
        P(None, "tp"),
        P(None, "tp"),
        P(),
        P(),
        P(),
        P(),
        P("ep", "tp", None, None),
        P("ep", "tp", None),
        P("ep", "tp"),
        P("tp", None),
        P(),
        P("ep", None),
        P("ep", None),
        P("ep", None, "tp"),
        P("ep", None, "tp"),
        P("ep", "tp", None),
        P(None, "tp"),
        P(None, "tp"),
        P("tp", None),
        P(),
    )
    out_specs = (P("ep", "tp"), P("ep", "tp", None, None), P("ep", "tp", None), P("ep", "tp"))
    return jax.shard_map(
        local, mesh=mesh, in_specs=in_specs, out_specs=out_specs, check_vma=False
    )
```
